32 devices in a mesh: sp: 16 (over z, y, x), tp: 2 (over core).
Axes of the slice: x: 2, y: 2, z: 4, core: 2. Of those that a mesh axis runs over, the one named last changes fastest.
Arguments:
- residual_in: bfloat16 [6144, 2048], P(('sp', 'tp')), may hold values from -6 to 6
- conv_values: bfloat16 [6144, 1024], P('sp', 'tp'), may hold values from -60 to 60
- conv_gates: bfloat16 [6144, 1024], P('sp', 'tp'), may hold values from -8 to 8
- conv_kernel: float32 [31, 1024], P(None, 'tp'), may hold values from -1 to 1
- conv_bias: float32 [1024], P('tp'), may hold values from -3 to 3
- chan_gain: float32 [1024], P('tp'), may hold values from 0.1 to 1.9
- chan_shift: float32 [1024], P('tp'), may hold values from -3 to 3
- out_weight: bfloat16 [1024, 2048], replicated, may hold values from -0.1875 to 0.1875
- norm_gain: float32 [2048], replicated, may hold values from 0.1 to 1.9
- route_ids: int32 [6144, 2], P(('sp', 'tp')), may hold values from 0 to 15, all different within a row; in each aligned block of 192 rows (0 to 191, 192 to 383, ...) at most 48 rows name the same one
- route_weights: float32 [6144, 2], P(('sp', 'tp')), may hold values from 0.25 to 1.5
- expert_gate: bfloat16 [16, 2048, 2048], P('sp', None, 'tp'), may hold values from -0.125 to 0.125
- expert_up: bfloat16 [16, 2048, 2048], P('sp', None, 'tp'), may hold values from -0.125 to 0.125
- expert_down: bfloat16 [16, 2048, 2048], P('sp', 'tp'), may hold values from -0.125 to 0.125
Outputs:
- layer_out: bfloat16 [6144, 2048], P(('sp', 'tp'))
The draws below stay inside these ranges and needn't reach their ends.
Inputs may be any that keep to these rules, and one draw needn't show every extreme that they name: `route_ids`: each row names 2 different experts. Among the rows of one device (aligned blocks of 192 rows) no expert is named by more than 48 rows, a bound that some block reaches.
All inputs are finite; a program needn't handle non-finite values.
Results may differ from the reference program's by a relative error of at most 0.014.
Values may be sent and summed in bfloat16 or wider, within the bound.
A program may use at most 128 MiB of HBM per device.

```python
import math
import jax
import jax.numpy as jnp
import numpy as np
from jax import lax

D = 2048
C = 1024
FF = 2048
KW = 31
TOPK = 2
ROWS = 192
TOKENS = 6144
EXPERTS = 16
CAP = 48
N_SP = 16
N_TP = 2


def draw_conv_values(key, part):
    keys = jax.random.split(jax.random.fold_in(key, 11), 3)
    columns = jnp.exp(jax.random.uniform(keys[0], (C,), jnp.float32, 0.0, math.log(10.0)))
    rowscale = jnp.exp(jax.random.uniform(keys[1], (TOKENS, 1), jnp.float32, 0.0, math.log(4.0)))
    base = jnp.clip(jax.random.normal(keys[2], (TOKENS, C), jnp.float32), -4.0, 4.0)
    values = jnp.clip(base * columns[None, :] * rowscale * 0.4, -60.0, 60.0)
    return values.astype(jnp.bfloat16)


def level_of(own_key, shape, pieces, smallest, high):
    def one(dim, blocks):
        draws = jax.random.uniform(jax.random.fold_in(jax.random.fold_in(own_key, 6), dim), (blocks,), jnp.float32, smallest / len(pieces), high / len(pieces))
        return jnp.repeat(jnp.exp(draws), shape[dim] // blocks).reshape((-1,) + (1,) * (len(shape) - dim - 1))

    level = one(*pieces[0])
    for cut in pieces[1:]:
        level = level * one(*cut)
    return level


def shared_out(rng, own, number, rows, amount, top, bound, lean):
    order = jax.random.permutation(rng, amount)
    packed, ordinary = portions_of(amount, rows * top, bound, lean, True), portions_of(amount, rows * top, bound, lean, False)
    places = jnp.arange(amount)

    def named(sizes, turn):
        used = int((sizes > 0).sum())
        fixed = max(1, used // 4)
        shifted = fixed + (places - fixed + turn * (used - fixed)) % max(1, amount - fixed)
        return jnp.zeros((amount,), jnp.int32).at[order[jnp.where(places < fixed, places, shifted)]].set(jnp.asarray(sizes, jnp.int32))

    sizes = jnp.where(number % 4 == 0, named(packed, number // 4), named(ordinary, number - number // 4 - 1))
    mixed = jax.random.permutation(jax.random.fold_in(own, 3), amount)
    giver, sink = mixed[0:amount // 2 * 2:2], mixed[1:amount // 2 * 2:2]
    margin = jnp.minimum(sizes[giver] - 1, bound - sizes[sink]) // 2
    margin = jnp.where((giver == order[0]) | (sink == order[0]) | (sizes[sink] == 0), 0, jnp.maximum(margin, 0))
    shifted = jax.random.randint(jax.random.fold_in(own, 4), (amount // 2,), 0, 1 << 20) % (margin + 1)
    sizes = sizes.at[giver].add(-shifted).at[sink].add(shifted)
    items = jnp.searchsorted(jnp.cumsum(sizes), jnp.arange(rows * top), side="right").astype(jnp.int32)
    grid = items.reshape(top, rows).T
    grid = grid[jax.random.permutation(jax.random.fold_in(own, 1), rows)]
    turn = jax.random.randint(jax.random.fold_in(own, 2), (rows, 1), 0, top)
    return jnp.take_along_axis(grid, (jnp.arange(top)[None, :] + turn) % top, axis=1)


def portions_of(number_of, total, bound, lean, full):
    loads = [(1 << 20) // math.isqrt(grade ** lean) + 1 for grade in range(1, number_of + 1)]
    largest = bound if full else min(bound, max(-(-total // number_of), total * loads[0] // sum(loads)))
    least = 1 if total - largest >= number_of - 1 else 0
    counts, spare = [largest] + [least] * (number_of - 1), total - largest - least * (number_of - 1)
    while spare > 0:
        movable = [i for i in range(1, number_of) if counts[i] < largest] or [i for i in range(1, number_of) if counts[i] < bound]
        pool, budget = sum([loads[i] for i in movable]), spare
        for i in movable:
            more = min(bound - counts[i], max(1, budget * loads[i] // pool), spare)
            counts[i] = counts[i] + more
            spare = spare - more
    return np.array(counts)


def centred(own_key, shape, deviation, most, pieces=(), held_as=jnp.bfloat16):
    loudness = level_of(own_key, shape, pieces, -0.22, 0.18) if pieces else 1.0
    result = jax.random.normal(own_key, shape, jnp.float32) * deviation * loudness
    return jnp.minimum(jnp.maximum(result, -most), most).astype(held_as)


def setup_inputs(seed: int = 0) -> dict:
    seeds = jax.random.split(jax.random.key(seed), 15)
    residual_in = centred(seeds[0], (TOKENS, D), 1.0, 6.0, ((0, 32),))
    conv_values = draw_conv_values(jax.random.fold_in(seeds[14], 71), 0)
    conv_gates = centred(seeds[2], (TOKENS, C), 1.5, 8.0, ((0, 16), (1, 2)))
    conv_kernel = centred(seeds[3], (KW, C), KW ** -0.5, 1.0, ((1, 2),), jnp.float32)
    conv_bias = centred(seeds[4], (C,), 0.5, 3.0, ((0, 2),), jnp.float32)
    chan_gain = jnp.clip(1.0 + 0.18 * jax.random.normal(seeds[5], (C,), jnp.float32), 0.1, 1.9)
    chan_shift = centred(seeds[6], (C,), 0.5, 3.0, ((0, 2),), jnp.float32)
    out_weight = centred(seeds[7], (C, D), C ** -0.5, 0.1875)
    norm_gain = jnp.clip(1.0 + 0.18 * jax.random.normal(seeds[8], (D,), jnp.float32), 0.1, 1.9)
    route_ids_keys = jax.random.split(jax.random.fold_in(seeds[9], 1), TOKENS // ROWS)
    route_ids_turns = jax.random.permutation(jax.random.fold_in(seeds[9], 3), TOKENS // ROWS)
    route_ids = jax.vmap(lambda own, number: shared_out(jax.random.fold_in(seeds[9], 2), own, number, ROWS, EXPERTS, TOPK, CAP, 2))(route_ids_keys, route_ids_turns).reshape((TOKENS, TOPK))
    route_weights = jnp.clip(0.25 + 1.25 * jax.random.uniform(seeds[10], (TOKENS, TOPK), jnp.float32) ** level_of(seeds[10], (TOKENS, TOPK), ((0, 32),), -0.2, 0.2), 0.25, 1.5)
    expert_gate = centred(seeds[11], (EXPERTS, D, FF), D ** -0.5, 0.125, ((0, 16), (2, 2)))
    expert_up = centred(seeds[12], (EXPERTS, D, FF), D ** -0.5, 0.125, ((0, 16), (2, 2)))
    expert_down = centred(seeds[13], (EXPERTS, FF, D), FF ** -0.5, 0.125, ((0, 16), (1, 2)))
    return {"residual_in": residual_in, "conv_values": conv_values, "conv_gates": conv_gates, "conv_kernel": conv_kernel, "conv_bias": conv_bias, "chan_gain": chan_gain, "chan_shift": chan_shift, "out_weight": out_weight, "norm_gain": norm_gain, "route_ids": route_ids, "route_weights": route_weights, "expert_gate": expert_gate, "expert_up": expert_up, "expert_down": expert_down}


def reference(residual_in, conv_values, conv_gates, conv_kernel, conv_bias, chan_gain, chan_shift, out_weight, norm_gain, route_ids, route_weights, expert_gate, expert_up, expert_down):
    seq_count = residual_in.shape[0]
    gated = (conv_values.astype(jnp.float32) * jax.nn.sigmoid(conv_gates.astype(jnp.float32))).astype(jnp.bfloat16)
    padded = jnp.concatenate([jnp.zeros((KW - 1, C), jnp.float32), gated.astype(jnp.float32)], 0)
    mixed = jnp.zeros((seq_count, C), jnp.float32) + conv_bias[None, :]
    for tap_index in range(KW):
        mixed = mixed + conv_kernel[tap_index][None, :] * padded[tap_index:tap_index + seq_count]
    center = lax.optimization_barrier(jnp.mean(mixed, 1, keepdims=True))
    spread = lax.optimization_barrier(jnp.mean(mixed * mixed, 1, keepdims=True)) - center * center
    normed = (mixed - center) * lax.rsqrt(spread + 1e-06) * chan_gain[None, :] + chan_shift[None, :]
    activated = jax.nn.silu(normed).astype(jnp.bfloat16)
    projected = jnp.dot(activated, out_weight, preferred_element_type=jnp.float32)
    after_mix = (residual_in.astype(jnp.float32) + projected).astype(jnp.bfloat16)
    after_f = after_mix.astype(jnp.float32)
    normal_rows = (after_f * lax.rsqrt(lax.optimization_barrier(jnp.mean(after_f * after_f, 1, keepdims=True)) + 1e-06) * norm_gain[None, :]).astype(jnp.bfloat16)
    flat_ids = route_ids.reshape(-1)
    flat_weights = route_weights.reshape(-1)
    most_rows = N_SP * N_TP * CAP
    half_width = FF // N_TP

    def per_expert(totals, inputs):
        gate_w, up_w, down_w, expert_index = inputs
        chosen = flat_ids == expert_index
        order = jnp.argsort(jnp.where(chosen, 0, 1).astype(jnp.int32), stable=True)[:most_rows].astype(jnp.int32)
        valid = chosen[order]
        token_index = (order // TOPK).astype(jnp.int32)
        picked = normal_rows[token_index]
        gate = jnp.dot(picked, gate_w, preferred_element_type=jnp.float32)
        upper = jnp.dot(picked, up_w, preferred_element_type=jnp.float32)
        hidden = (jax.nn.silu(gate) * upper).astype(jnp.bfloat16)
        summed = jnp.zeros((most_rows, D), jnp.float32)
        for half_index in range(N_TP):
            partial_out = jnp.dot(hidden[:, half_index * half_width:(half_index + 1) * half_width], down_w[half_index * half_width:(half_index + 1) * half_width], preferred_element_type=jnp.float32)
            partial_out = lax.optimization_barrier(partial_out.astype(jnp.bfloat16))
            summed = summed + partial_out.astype(jnp.float32)
        expert_out = summed.astype(jnp.bfloat16).astype(jnp.float32)
        weight = jnp.where(valid, flat_weights[order], 0.0)
        totals = totals.at[token_index].add(weight[:, None] * expert_out)
        return (totals, None)
    totals, unused = lax.scan(per_expert, jnp.zeros((seq_count, D), jnp.float32), (expert_gate, expert_up, expert_down, jnp.arange(EXPERTS, dtype=jnp.int32)))
    return (after_f + totals).astype(jnp.bfloat16)
```

```python
import functools

import jax
import jax.numpy as jnp
from jax import lax
from jax.experimental import pallas as pl
from jax.experimental.pallas import tpu as pltpu
from jax.sharding import PartitionSpec as P

GROUPS = 4
ORDER = (0, 2, 1, 3)
MESH = pl.DeviceIdType.MESH


def flipped(index, offset):
    result, bit = index, 1
    while bit <= offset:
        if offset & bit:
            result = result + bit * (1 - 2 * ((index // bit) % 2))
        bit *= 2
    return result


def experts_kernel(
    count, cap, send, gate_in, up_in, down_in, out,
    rows, part, given, total, hidden, gate_w, up_w, down_w,
    sent, came, back_sent, back_came, pair_sent, pair_came, part_sent, part_came, loaded,
):
    me, other = lax.axis_index("sp"), 1 - lax.axis_index("tp")
    per_group = count // GROUPS
    half = per_group * cap
    loads = [
        pltpu.make_async_copy(source.at[0], target, loaded.at[number])
        for number, (source, target) in enumerate(
            ((gate_in, gate_w), (up_in, up_w), (down_in, down_w))
        )
    ]
    for load in loads:
        load.start()

    barrier = pltpu.get_barrier_semaphore()
    for offset in range(1, count):
        pl.semaphore_signal(
            barrier, inc=1, device_id={"sp": flipped(me, offset)}, device_id_type=MESH
        )
    pl.semaphore_signal(barrier, inc=1, device_id={"tp": other}, device_id_type=MESH)
    pl.semaphore_wait(barrier, count)

    outgoing = {}
    for group in ORDER:
        for place in range(per_group):
            offset = group * per_group + place
            source = send.at[pl.ds(offset * cap, cap)]
            target = rows.at[group, pl.ds(place * cap, cap)]
            if offset == 0:
                copy = pltpu.make_async_copy(source, target, sent.at[0])
            else:
                copy = pltpu.make_async_remote_copy(
                    src_ref=source,
                    dst_ref=target,
                    send_sem=sent.at[offset],
                    recv_sem=came.at[offset],
                    device_id={"sp": flipped(me, offset)},
                    device_id_type=MESH,
                )
            copy.start()
            outgoing[offset] = copy

    late, returning = [], {}
    for turn, group in enumerate(ORDER):
        for place in range(per_group):
            offset = group * per_group + place
            if offset == 0:
                outgoing[0].wait()
            else:
                outgoing[offset].wait_recv()
        pair = pltpu.make_async_remote_copy(
            src_ref=rows.at[group, pl.ds(0, half)],
            dst_ref=rows.at[group, pl.ds(half, half)],
            send_sem=pair_sent.at[group],
            recv_sem=pair_came.at[group],
            device_id={"tp": other},
            device_id_type=MESH,
        )
        pair.start()
        late.append(pair)
        if turn == 0:
            for load in loads:
                load.wait()
        pair.wait_recv()

        wide = min(256, gate_w.shape[1])

        def first(step, carry, group=group):
            columns = pl.ds(pl.multiple_of(step * wide, wide), wide)
            gate = jnp.dot(rows[group], gate_w[:, columns], preferred_element_type=jnp.float32)
            upper = jnp.dot(rows[group], up_w[:, columns], preferred_element_type=jnp.float32)
            hidden[:, columns] = (jax.nn.silu(gate) * upper).astype(jnp.bfloat16)
            return carry

        lax.fori_loop(0, gate_w.shape[1] // wide, first, 0)

        def second(step, carry, group=group):
            columns = pl.ds(pl.multiple_of(step * wide, wide), wide)
            part[group, :, columns] = jnp.dot(
                hidden[...], down_w[:, columns], preferred_element_type=jnp.float32
            ).astype(jnp.bfloat16)
            return carry

        lax.fori_loop(0, down_w.shape[1] // wide, second, 0)

        share = pltpu.make_async_remote_copy(
            src_ref=part.at[group, pl.ds(half, half)],
            dst_ref=given.at[group],
            send_sem=part_sent.at[group],
            recv_sem=part_came.at[group],
            device_id={"tp": other},
            device_id_type=MESH,
        )
        share.start()
        late.append(share)
        share.wait_recv()
        total[group] = (
            part[group, pl.ds(0, half)].astype(jnp.float32) + given[group].astype(jnp.float32)
        ).astype(jnp.bfloat16)
        for place in range(per_group):
            offset = group * per_group + place
            source = total.at[group, pl.ds(place * cap, cap)]
            target = out.at[pl.ds(offset * cap, cap)]
            if offset == 0:
                copy = pltpu.make_async_copy(source, target, back_sent.at[0])
            else:
                copy = pltpu.make_async_remote_copy(
                    src_ref=source,
                    dst_ref=target,
                    send_sem=back_sent.at[offset],
                    recv_sem=back_came.at[offset],
                    device_id={"sp": flipped(me, offset)},
                    device_id_type=MESH,
                )
            copy.start()
            returning[offset] = copy

    for offset in range(1, count):
        outgoing[offset].wait_send()
    for copy in late:
        copy.wait_send()
    for offset in range(count):
        returning[offset].wait()


def run_experts(sendable, expert_gate, expert_up, expert_down, count, cap):
    width, units = expert_gate.shape[1], expert_gate.shape[2]
    half = count // GROUPS * cap
    grouped = pltpu.SemaphoreType.DMA((GROUPS,))
    each = pltpu.SemaphoreType.DMA((count,))
    vmem = pl.BlockSpec(memory_space=pltpu.VMEM)
    anywhere = pl.BlockSpec(memory_space=pl.ANY)
    held = jnp.bfloat16
    return pl.pallas_call(
        functools.partial(experts_kernel, count, cap),
        out_shape=jax.ShapeDtypeStruct(sendable.shape, held),
        in_specs=[vmem, anywhere, anywhere, anywhere],
        out_specs=vmem,
        scratch_shapes=[
            pltpu.VMEM((GROUPS, 2 * half, width), held),
            pltpu.VMEM((GROUPS, 2 * half, width), held),
            pltpu.VMEM((GROUPS, half, width), held),
            pltpu.VMEM((GROUPS, half, width), held),
            pltpu.VMEM((2 * half, units), held),
            pltpu.VMEM((width, units), held),
            pltpu.VMEM((width, units), held),
            pltpu.VMEM((units, width), held),
            each, each, each, each, grouped, grouped, grouped, grouped,
            pltpu.SemaphoreType.DMA((3,)),
        ],
        compiler_params=pltpu.CompilerParams(
            collective_id=0, has_side_effects=True, vmem_limit_bytes=60 * 1024 * 1024
        ),
    )(sendable, expert_gate, expert_up, expert_down)


def from_behind(value, axis, steps):
    count = lax.axis_size(axis)
    first, last = (max(0, -steps), min(count, count - steps))
    return lax.ppermute(value, axis, [(source, source + steps) for source in range(first, last)])


def swap(value, axis, offset):
    count = lax.axis_size(axis)
    return lax.ppermute(value, axis, [(source, source ^ offset) for source in range(count)])


def on_device(
    residual_in,
    conv_values,
    conv_gates,
    conv_kernel,
    conv_bias,
    chan_gain,
    chan_shift,
    out_weight,
    norm_gain,
    route_ids,
    route_weights,
    expert_gate,
    expert_up,
    expert_down,
):
    taps_count = conv_kernel.shape[0]
    tok_count, local_chan = conv_values.shape
    tp_count = lax.axis_size("tp")
    all_chan = local_chan * tp_count
    core = lax.axis_index("tp")
    gated = (
        conv_values.astype(jnp.float32) * jax.nn.sigmoid(conv_gates.astype(jnp.float32))
    ).astype(jnp.bfloat16)
    earlier = from_behind(gated[tok_count - (taps_count - 1) :], "sp", 1)
    extended = jnp.concatenate([earlier, gated], 0).astype(jnp.float32)
    mixed = jnp.zeros((tok_count, local_chan), jnp.float32) + conv_bias[None, :]
    for tap_index in range(taps_count):
        mixed = (
            mixed + conv_kernel[tap_index][None, :] * extended[tap_index : tap_index + tok_count]
        )
    sums = jnp.stack([jnp.sum(mixed, 1), jnp.sum(mixed * mixed, 1)])
    sums = sums + swap(sums, "tp", 1)
    center = (sums[0] / all_chan)[:, None]
    spread = (sums[1] / all_chan)[:, None] - center * center
    normed = (mixed - center) * lax.rsqrt(spread + 1e-06) * chan_gain[None, :] + chan_shift[None, :]
    activated = jax.nn.silu(normed).astype(jnp.bfloat16)
    row_count = tok_count // tp_count
    low, high = activated[:row_count], activated[row_count:]
    kept = jnp.where(core == 0, low, high)
    given = swap(jnp.where(core == 0, high, low), "tp", 1)
    regrouped = jnp.concatenate(
        [jnp.where(core == 0, kept, given), jnp.where(core == 0, given, kept)], 1
    )
    projected = jnp.dot(regrouped, out_weight, preferred_element_type=jnp.float32)
    after_f = (residual_in.astype(jnp.float32) + projected).astype(jnp.bfloat16).astype(jnp.float32)
    normal_rows = (
        after_f
        * lax.rsqrt(jnp.mean(after_f * after_f, 1, keepdims=True) + 1e-06)
        * norm_gain[None, :]
    ).astype(jnp.bfloat16)
    sp_count = lax.axis_size("sp")
    experts_all = expert_gate.shape[0] * sp_count
    choose_count = route_ids.shape[1]
    slot_cap = max(2, (2 * choose_count * row_count + experts_all - 1) // experts_all)
    slot_cap = (slot_cap + 15) // 16 * 16
    onehot = (
        route_ids.reshape(-1)[:, None] == jnp.arange(experts_all, dtype=jnp.int32)[None, :]
    ).astype(jnp.int32)
    before = jnp.cumsum(onehot, 0) - onehot
    ranking = jnp.sum(before * onehot, 1).reshape(row_count, choose_count)
    slot_ids = (route_ids ^ lax.axis_index("sp")) * slot_cap + ranking
    positions = lax.broadcasted_iota(jnp.int32, (experts_all * slot_cap, 1, 1), 0)
    dispatch = jnp.any(positions == slot_ids[None, :, :], axis=2).astype(jnp.bfloat16)
    columns = lax.broadcasted_iota(jnp.int32, (1, 1, experts_all * slot_cap), 2)
    weighting = jnp.sum(
        jnp.where(columns == slot_ids[:, :, None], route_weights[:, :, None], 0.0), 1
    )
    coarse_f = lax.reduce_precision(weighting, 8, 7)
    coarse = coarse_f.astype(jnp.bfloat16)
    fine = (weighting - coarse_f).astype(jnp.bfloat16)
    sendable = jnp.dot(dispatch, normal_rows, preferred_element_type=jnp.float32).astype(
        jnp.bfloat16
    )
    flat_out = run_experts(sendable, expert_gate, expert_up, expert_down, sp_count, slot_cap)
    combined = (
        after_f
        + jnp.dot(coarse, flat_out, preferred_element_type=jnp.float32)
        + jnp.dot(fine, flat_out, preferred_element_type=jnp.float32)
    )
    return combined.astype(jnp.bfloat16)


def solution(mesh):
    placed = (
        P(("sp", "tp"), None),
        P("sp", "tp"),
        P("sp", "tp"),
        P(None, "tp"),
        P("tp"),
        P("tp"),
        P("tp"),
        P(),
        P(),
        P(("sp", "tp"), None),
        P(("sp", "tp"), None),
        P("sp", None, "tp"),
        P("sp", None, "tp"),
        P("sp", "tp", None),
    )
    return jax.shard_map(
        on_device, mesh=mesh, in_specs=placed, out_specs=P(("sp", "tp"), None), check_vma=False
    )
```
